32 devices in a mesh: fs: 8 (over z, y), tp: 4 (over x, core).
Axes of the slice: x: 2, y: 2, z: 4, core: 2. Of those that a mesh axis runs over, the one named last changes fastest.
Arguments:
- tokens: bfloat16 [8, 384, 2048], P('fs', None, 'tp'), may hold values from -16 to 16
- first_gate: bfloat16 [2048, 6144], P('fs', 'tp'), may hold values from -0.125 to 0.125
- first_up: bfloat16 [2048, 6144], P('fs', 'tp'), may hold values from -0.125 to 0.125
- first_down: bfloat16 [6144, 2048], P('tp', 'fs'), may hold values from -0.078125 to 0.078125
- first_gain: bfloat16 [2048], P('tp'), may hold values from 0.099609375 to 1.8984375
- glu_value: bfloat16 [2048, 1024], P('fs', 'tp'), may hold values from -0.125 to 0.125
- glu_gate: bfloat16 [2048, 1024], P('fs', 'tp'), may hold values from -0.125 to 0.125
- conv_taps: bfloat16 [31, 1024], P(None, 'tp'), may hold values from -3 to 3
- conv_gain: bfloat16 [1024], P('tp'), may hold values from 0.099609375 to 1.8984375
- conv_proj: bfloat16 [1024, 2048], P('tp', 'fs'), may hold values from -0.1875 to 0.1875
- second_gain: bfloat16 [2048], P('tp'), may hold values from 0.099609375 to 1.8984375
- last_gate: bfloat16 [2048, 6144], P('fs', 'tp'), may hold values from -0.125 to 0.125
- last_up: bfloat16 [2048, 6144], P('fs', 'tp'), may hold values from -0.125 to 0.125
- last_down: bfloat16 [6144, 2048], P('tp', 'fs'), may hold values from -0.078125 to 0.078125
- third_gain: bfloat16 [2048], P('tp'), may hold values from 0.099609375 to 1.8984375
Outputs:
- layer_out: bfloat16 [8, 384, 2048], P('fs', None, 'tp')
The draws below stay inside these ranges and needn't reach their ends.
All inputs are finite; a program needn't handle non-finite values.
Results may differ from the reference program's by a relative error of at most 0.015.
Values may be sent and summed in bfloat16 or wider, within the bound.
A program may use at most 64 MiB of HBM per device.

```python
import jax
import jax.numpy as jnp
from jax import lax

D = 2048
FF = 6144
CONV = 1024
KERNEL = 31
LEN = 384
SEQS = 8
N_TP = 4


def draw_tokens(key, part):
    values = jnp.clip(jax.random.normal(key, (SEQS, LEN, D), jnp.float32), -5.0, 5.0)
    rising = 10.0 ** (jnp.arange(D, dtype=jnp.float32) / D - 0.5)
    return (values * rising).astype(jnp.bfloat16)


def draw_conv_taps(key, part):
    values = jnp.clip(jax.random.normal(key, (KERNEL, CONV), jnp.float32), -5.0, 5.0)
    rising = 10.0 ** (jnp.arange(CONV, dtype=jnp.float32) / CONV - 0.5)
    return (values * rising / jnp.sqrt(1.0 * KERNEL)).astype(jnp.bfloat16)


def shard_levels(own_key, extent, pieces, low, high):
    level, own = 1.0, jax.random.fold_in(own_key, 6)
    for axis_at, blocks in pieces:
        heights = jnp.exp(jax.random.uniform(jax.random.fold_in(own, axis_at), (blocks,), jnp.float32, low / len(pieces), high / len(pieces)))
        level = level * jnp.repeat(heights, extent[axis_at] // blocks).reshape([-1 if axis == axis_at else 1 for axis in range(len(extent))])
    return level


def centred(stream_key, extent, scale, bound, pieces=(), kind=jnp.bfloat16):
    values = scale * jax.random.normal(stream_key, extent, jnp.float32)
    if pieces:
        values = values * shard_levels(stream_key, extent, pieces, -0.22, 0.18)
    return jnp.clip(values, -bound, bound).astype(kind)


def setup_inputs(seed: int = 0) -> dict:
    streams_of = jax.random.split(jax.random.key(seed), 16)
    tokens = draw_tokens(jax.random.fold_in(streams_of[15], 71), 0)
    first_gate = centred(streams_of[1], (D, FF), D ** -0.5, 0.125, ((0, 8), (1, 4)))
    first_up = centred(streams_of[2], (D, FF), D ** -0.5, 0.125, ((0, 8), (1, 4)))
    first_down = centred(streams_of[3], (FF, D), FF ** -0.5, 0.078125, ((0, 4), (1, 8)))
    first_gain = jnp.clip(1.0 + 0.18 * jax.random.normal(streams_of[4], (D,), jnp.float32), 0.099609375, 1.8984375).astype(jnp.bfloat16)
    glu_value = centred(streams_of[5], (D, CONV), D ** -0.5, 0.125, ((0, 8), (1, 4)))
    glu_gate = centred(streams_of[6], (D, CONV), D ** -0.5, 0.125, ((0, 8), (1, 4)))
    conv_taps = draw_conv_taps(jax.random.fold_in(streams_of[15], 71), 0)
    conv_gain = jnp.clip(1.0 + 0.18 * jax.random.normal(streams_of[8], (CONV,), jnp.float32), 0.099609375, 1.8984375).astype(jnp.bfloat16)
    conv_proj = centred(streams_of[9], (CONV, D), CONV ** -0.5, 0.1875, ((0, 4), (1, 8)))
    second_gain = jnp.clip(1.0 + 0.18 * jax.random.normal(streams_of[10], (D,), jnp.float32), 0.099609375, 1.8984375).astype(jnp.bfloat16)
    last_gate = centred(streams_of[11], (D, FF), D ** -0.5, 0.125, ((0, 8), (1, 4)))
    last_up = centred(streams_of[12], (D, FF), D ** -0.5, 0.125, ((0, 8), (1, 4)))
    last_down = centred(streams_of[13], (FF, D), FF ** -0.5, 0.078125, ((0, 4), (1, 8)))
    third_gain = jnp.clip(1.0 + 0.18 * jax.random.normal(streams_of[14], (D,), jnp.float32), 0.099609375, 1.8984375).astype(jnp.bfloat16)
    return dict(tokens=tokens, first_gate=first_gate, first_up=first_up, first_down=first_down, first_gain=first_gain, glu_value=glu_value, glu_gate=glu_gate, conv_taps=conv_taps, conv_gain=conv_gain, conv_proj=conv_proj, second_gain=second_gain, last_gate=last_gate, last_up=last_up, last_down=last_down, third_gain=third_gain)


ALPHA = 2.0 ** 0.25
EPSILON = 1e-05

def norm_rows(values, gain):
    center = lax.optimization_barrier(jnp.mean(values, axis=-1, keepdims=True))
    spread = lax.optimization_barrier(jnp.mean(jnp.square(values - center), axis=-1, keepdims=True))
    return (values - center) * lax.rsqrt(spread + EPSILON) * gain.astype(jnp.float32)

def split_sum(hidden, weight):
    blocks = hidden.shape[1] // N_TP
    left = hidden.reshape(hidden.shape[0], N_TP, blocks).astype(jnp.float32)
    right = weight.reshape(N_TP, blocks, weight.shape[1]).astype(jnp.float32)
    parts = jnp.einsum('rbf,bfd->brd', left, right)
    parts = lax.optimization_barrier(parts.astype(jnp.bfloat16))
    return lax.optimization_barrier(jnp.sum(parts.astype(jnp.float32), axis=0))

def feed_forward(current, w_gate, w_up, w_down):
    gate = jnp.dot(current, w_gate, preferred_element_type=jnp.float32)
    upward = jnp.dot(current, w_up, preferred_element_type=jnp.float32)
    hidden = (jax.nn.silu(gate) * upward).astype(jnp.bfloat16)
    return split_sum(hidden, w_down)

def post_norm(current, branch, weight, gain):
    mixed = ALPHA * current.astype(jnp.float32) + weight * branch
    return norm_rows(mixed, gain).astype(jnp.bfloat16)

def conv_module(current, glu_value, glu_gate, conv_taps, conv_gain, conv_proj):
    value = jnp.dot(current, glu_value, preferred_element_type=jnp.float32)
    gate = jnp.dot(current, glu_gate, preferred_element_type=jnp.float32)
    gated = value * jax.nn.sigmoid(gate)
    reach = (conv_taps.shape[0] - 1) // 2
    length = gated.shape[0]
    padded = jnp.pad(gated, ((reach, reach), (0, 0)))
    taps = conv_taps.astype(jnp.float32)
    mixed = jnp.zeros_like(gated)
    for tap_index in range(conv_taps.shape[0]):
        mixed = mixed + taps[tap_index] * padded[tap_index:tap_index + length]
    normed = jax.nn.silu(norm_rows(mixed, conv_gain)).astype(jnp.bfloat16)
    return split_sum(normed, conv_proj)

def reference(tokens, first_gate, first_up, first_down, first_gain, glu_value, glu_gate, conv_taps, conv_gain, conv_proj, second_gain, last_gate, last_up, last_down, third_gain):

    def one_sequence(current):
        first = post_norm(current, feed_forward(current, first_gate, first_up, first_down), 0.5, first_gain)
        second = post_norm(first, conv_module(first, glu_value, glu_gate, conv_taps, conv_gain, conv_proj), 1.0, second_gain)
        return post_norm(second, feed_forward(second, last_gate, last_up, last_down), 0.5, third_gain)
    return lax.map(one_sequence, tokens)
```

```python
import functools

import jax
import jax.numpy as jnp
from jax import lax
from jax.experimental import pallas as pl
from jax.experimental.pallas import tpu as pltpu
from jax.sharding import PartitionSpec as P

ALPHA = 2.0**0.25
EPSILON = 1e-05
MESH = pl.DeviceIdType.MESH
F32 = jnp.float32
BF16 = jnp.bfloat16


def plan_pieces(parts):
    pieces = []
    for matrix, (rows, cuts) in enumerate(parts):
        start = 0
        for size, swapped in cuts(rows):
            pieces.append((matrix, start, size, swapped))
            start += size
    return pieces


def halves(rows):
    return [(rows // 2, False), (rows // 2, False)]


def whole(rows):
    return [(rows, True)]


def half_swapped(rows):
    return [(rows // 2, True), (rows // 2, False)]


def layer_kernel(
    n_fs,
    n_tp,
    n_y,
    pieces,
    tokens_ref,
    *refs,
):
    weights = refs[:9]
    first_gain, conv_taps, conv_gain, second_gain, third_gain = refs[9:14]
    out_ref = refs[14]
    bufs = refs[15:24]
    (xg, rs, send_buf, hidden, current, conv_in, acted, stat, z_s, z_r, y_s, y_r, loc_s, ag_s, ag_r, rs_s, rs_r, st_s, st_r) = refs[24:]

    n_z = n_fs // n_y
    fs = lax.axis_index("fs")
    tp = lax.axis_index("tp")
    z, y = fs // n_y, fs % n_y
    length, width = tokens_ref.shape
    features = width * n_tp

    barrier = pltpu.get_barrier_semaphore()
    for other in range(n_fs):
        @pl.when(other != fs)
        def _():
            pl.semaphore_signal(barrier, inc=1, device_id=(other, tp), device_id_type=MESH)
    for step in range(1, n_tp):
        pl.semaphore_signal(barrier, inc=1, device_id=(fs, (tp + step) % n_tp), device_id_type=MESH)
    pl.semaphore_wait(barrier, n_fs - 1 + n_tp - 1)

    pending = []

    def slot(matrix, start, size, block):
        buf = bufs[matrix]
        if len(buf.shape) == 2:
            rows = weights[matrix].shape[0]
            return buf.at[pl.ds(pl.multiple_of(block * rows + start, 8), size)]
        return buf.at[block, pl.ds(start, size)]

    def remote(src, dst, s, r, dest):
        return pltpu.make_async_remote_copy(
            src_ref=src, dst_ref=dst, send_sem=s, recv_sem=r, device_id=dest, device_id_type=MESH
        )

    def axes(swapped):
        major, minor = (z, n_z, n_y), (y, n_y, 1)
        return (minor, major) if swapped else (major, minor)

    def when(cond, fn):
        pl.when(cond)(fn)

    def place(c, k, d, side):
        _, (_, extent, _) = axes(pieces[c][3])
        return (k * (extent - 1) + d - 1) * 2 + side

    def second_send(c, k, block, src):
        matrix, start, size, swapped = pieces[c]
        _, (pos, extent, stride) = axes(swapped)
        for side, sign in ((0, 1), (1, -1)):
            ok = pos < extent - 1 if side == 0 else pos > 0

            def go(side=side, sign=sign):
                i = place(c, k, 1, side)
                remote(src, slot(matrix, start, size, block), y_s.at[c, i], y_r.at[c, i], (fs + sign * stride, tp)).start()

            def done(side=side, sign=sign):
                i = place(c, k, 1, side)
                remote(src, slot(matrix, start, size, block), y_s.at[c, i], y_r.at[c, i], (fs + sign * stride, tp)).wait_send()

            when(ok, go)
            pending.append((ok, done))

    def own(c):
        matrix, start, size, swapped = pieces[c]
        src = weights[matrix].at[pl.ds(start, size)]
        (pos, extent, stride), _ = axes(swapped)
        for side, sign in ((0, 1), (1, -1)):
            ok = pos < extent - 1 if side == 0 else pos > 0

            def copy(side=side, sign=sign):
                return remote(src, slot(matrix, start, size, fs), z_s.at[c, side], z_r.at[c, side], (fs + sign * stride, tp))

            when(ok, lambda copy=copy: copy().start())
            pending.append((ok, lambda copy=copy: copy().wait_send()))
        second_send(c, 0, fs, src)
        pltpu.make_async_copy(src, slot(matrix, start, size, fs), loc_s.at[c]).start()

    def first_axis(c):
        matrix, start, size, swapped = pieces[c]
        (pos, extent, stride), _ = axes(swapped)
        for d in range(1, extent):
            for side, sign in ((0, 1), (1, -1)):
                here = pos - sign * d >= 0 if side == 0 else pos + d < extent
                onward = here & (pos < extent - 1 if side == 0 else pos > 0)
                block = fs - sign * d * stride
                i = (d - 1) * 2 + side

                def arrive(block=block, i=i):
                    dst = slot(matrix, start, size, block)
                    remote(dst, dst, z_s.at[c, i], z_r.at[c, i], (fs, tp)).wait_recv()

                when(here, arrive)
                if d < extent - 1:
                    def copy(block=block, i=i, sign=sign):
                        dst = slot(matrix, start, size, block)
                        return remote(dst, dst, z_s.at[c, i + 2], z_r.at[c, i + 2], (fs + sign * stride, tp))

                    when(onward, lambda copy=copy: copy().start())
                    pending.append((onward, lambda copy=copy: copy().wait_send()))
                k = 1 + i
                _, (pos2, extent2, stride2) = axes(swapped)
                for side2, sign2 in ((0, 1), (1, -1)):
                    ok = here & (pos2 < extent2 - 1 if side2 == 0 else pos2 > 0)

                    def copy2(block=block, k=k, side2=side2, sign2=sign2, stride2=stride2):
                        j = place(c, k, 1, side2)
                        dst = slot(matrix, start, size, block)
                        return remote(dst, dst, y_s.at[c, j], y_r.at[c, j], (fs + sign2 * stride2, tp))

                    when(ok, lambda copy2=copy2: copy2().start())
                    pending.append((ok, lambda copy2=copy2: copy2().wait_send()))
                yield

    def second_axis(c):
        matrix, start, size, swapped = pieces[c]
        (pos, extent, stride), (pos2, extent2, stride2) = axes(swapped)
        origins = [(0, None, 0)] + [
            (1 + (d - 1) * 2 + side, side, d) for d in range(1, extent) for side in (0, 1)
        ]
        for d2 in range(1, extent2):
            for k, side, d in origins:
                if side is None:
                    here, first = True, fs
                else:
                    sign = 1 if side == 0 else -1
                    here = pos - d >= 0 if side == 0 else pos + d < extent
                    first = fs - sign * d * stride
                for side2, sign2 in ((0, 1), (1, -1)):
                    got = here & (pos2 - d2 >= 0 if side2 == 0 else pos2 + d2 < extent2)
                    block = first - sign2 * d2 * stride2
                    i = place(c, k, d2, side2)

                    def arrive(block=block, i=i):
                        dst = slot(matrix, start, size, block)
                        remote(dst, dst, y_s.at[c, i], y_r.at[c, i], (fs, tp)).wait_recv()

                    when(got, arrive)
                    if d2 < extent2 - 1:
                        ok = got & (pos2 < extent2 - 1 if side2 == 0 else pos2 > 0)

                        def copy(block=block, i=i, sign2=sign2):
                            dst = slot(matrix, start, size, block)
                            return remote(dst, dst, y_s.at[c, i + 2], y_r.at[c, i + 2], (fs + sign2 * stride2, tp))

                        when(ok, lambda copy=copy: copy().start())
                        pending.append((ok, lambda copy=copy: copy().wait_send()))
            yield
        pltpu.make_async_copy(
            weights[matrix].at[pl.ds(start, size)], slot(matrix, start, size, fs), loc_s.at[c]
        ).wait()

    landed = [0]

    def stream():
        count = len(pieces)
        for c in range(min(2, count)):
            own(c)
        yield
        yield from first_axis(0)
        for c in range(count):
            if c + 2 < count:
                own(c + 2)
            if c + 1 < count:
                yield from first_axis(c + 1)
            yield from second_axis(c)
            landed[0] = c + 1
            yield

    pump_state = stream()

    def pump(steps):
        for _ in range(steps):
            next(pump_state, None)

    def until(matrix):
        need = max(i for i, piece in enumerate(pieces) if piece[0] == matrix) + 1
        while landed[0] < need:
            next(pump_state)

    def my_columns():
        return pl.ds(pl.multiple_of(tp * width, 128), width)

    def gather_start(phase, src):
        dst = xg.at[phase, :, my_columns()]
        for step in range(1, n_tp):
            i = step - 1
            remote(src, dst, ag_s.at[phase, i], ag_r.at[phase, i], (fs, (tp + step) % n_tp)).start()

    def gather_wait(phase, src):
        for step in range(1, n_tp):
            i = step - 1
            remote(src, src, ag_s.at[phase, i], ag_r.at[phase, i], (fs, tp)).wait()

    def scatter_start(phase):
        for step in range(1, n_tp):
            i = step - 1
            to = (tp + step) % n_tp
            remote(send_buf.at[to], rs.at[phase, i], rs_s.at[phase, i], rs_r.at[phase, i], (fs, to)).start()

    def scatter_wait(phase):
        for step in range(1, n_tp):
            i = step - 1
            remote(send_buf.at[0], rs.at[phase, i], rs_s.at[phase, i], rs_r.at[phase, i], (fs, tp)).wait()
        total = send_buf[pl.ds(tp, 1)][0].astype(F32)
        for i in range(n_tp - 1):
            total = total + rs[phase, i].astype(F32)
        return total

    def stats_start(phase, values):
        sums = jnp.sum(values, axis=-1, keepdims=True)
        squares = jnp.sum(values * values, axis=-1, keepdims=True)
        lane = lax.broadcasted_iota(jnp.int32, (values.shape[0], 128), 1)
        both = jnp.where(lane == 0, sums, jnp.where(lane == 1, squares, 0.0))
        stat[phase, n_tp - 1] = both.T[:8]
        for step in range(1, n_tp):
            i = step - 1
            remote(
                stat.at[phase, n_tp - 1], stat.at[phase, i], st_s.at[phase, i], st_r.at[phase, i],
                (fs, (tp + step) % n_tp),
            ).start()

    def stats_wait(phase, all_width):
        for step in range(1, n_tp):
            i = step - 1
            remote(
                stat.at[phase, n_tp - 1], stat.at[phase, i], st_s.at[phase, i], st_r.at[phase, i], (fs, tp)
            ).wait()
        total = stat[phase, 0]
        for i in range(1, n_tp):
            total = total + stat[phase, i]
        both = jnp.concatenate([total] * 16, axis=0).T
        center = both[:, 0:1] / all_width
        spread = both[:, 1:2] / all_width - center * center
        return center, lax.rsqrt(spread + EPSILON)

    def ffn_hidden(phase, gate, up):
        tile = min(256, gate.shape[1])

        def step(j, carry):
            cols = pl.ds(pl.multiple_of(j * tile, 128), tile)
            held = xg[phase]
            g = jnp.dot(held, gate[:, cols], preferred_element_type=F32)
            u = jnp.dot(held, up[:, cols], preferred_element_type=F32)
            hidden[:, cols] = (g * jax.nn.sigmoid(g) * u).astype(BF16)
            return carry

        lax.fori_loop(0, gate.shape[1] // tile, step, 0)

    def project(source, buf):
        part = buf.shape[2]
        per = width // part

        def step(t, carry):
            held = source[...]
            for q in range(per):
                send_buf[t, :, q * part : (q + 1) * part] = jnp.dot(
                    held, buf[t * per + q], preferred_element_type=F32
                ).astype(BF16)
            return carry

        lax.fori_loop(0, n_tp, step, 0)

    pump(1)
    xg[0, :, my_columns()] = tokens_ref[...]
    gather_start(0, tokens_ref)
    until(0)
    gather_wait(0, tokens_ref)
    until(1)
    ffn_hidden(0, bufs[0], bufs[1])
    until(2)
    project(hidden, bufs[2])
    scatter_start(0)
    pump(6)
    mixed = ALPHA * tokens_ref[...].astype(F32) + 0.5 * scatter_wait(0)
    current[...] = mixed
    stats_start(0, mixed)
    pump(4)
    center, scale = stats_wait(0, features)
    first = ((current[...] - center) * scale * first_gain[...].astype(F32)).astype(BF16)
    out_ref[...] = first
    xg[1, :, my_columns()] = first
    gather_start(1, out_ref)
    until(4)
    gather_wait(1, out_ref)

    channels = acted.shape[1]
    taps = conv_taps.shape[0]
    reach = (taps - 1) // 2
    margin = (conv_in.shape[0] - length) // 2
    held = xg[1]
    value = jnp.dot(held, bufs[3][...], preferred_element_type=F32)
    gate = jnp.dot(held, bufs[4][...], preferred_element_type=F32)
    conv_in[0:margin] = jnp.zeros((margin, channels), F32)
    conv_in[margin + length :] = jnp.zeros((margin, channels), F32)
    conv_in[margin : margin + length] = value * jax.nn.sigmoid(gate)
    pump(2)
    rows_each = length // 4
    for low in range(0, length, rows_each):
        for left in range(0, channels, 128):
            cols = slice(left, left + 128)
            total = jnp.zeros((rows_each, 128), F32)
            for tap in range(taps):
                start = margin - reach + low + tap
                total = total + conv_taps[tap : tap + 1, cols].astype(F32) * conv_in[start : start + rows_each, cols]
            current[low : low + rows_each, cols] = total
    stats_start(1, current[:, 0:channels])
    pump(4)
    center, scale = stats_wait(1, channels * n_tp)
    normed = (current[:, 0:channels] - center) * scale * conv_gain[...].astype(F32)
    acted[...] = (normed * jax.nn.sigmoid(normed)).astype(BF16)
    until(5)
    project(acted, bufs[5])
    scatter_start(1)
    pump(4)
    mixed = ALPHA * out_ref[...].astype(F32) + scatter_wait(1)
    current[...] = mixed
    stats_start(2, mixed)
    pump(4)
    center, scale = stats_wait(2, features)
    second = ((current[...] - center) * scale * second_gain[...].astype(F32)).astype(BF16)
    out_ref[...] = second
    xg[2, :, my_columns()] = second
    gather_start(2, out_ref)
    pump(4)
    gather_wait(2, out_ref)

    until(7)
    ffn_hidden(2, bufs[6], bufs[7])
    until(8)
    project(hidden, bufs[8])
    scatter_start(2)
    for _ in pump_state:
        pass
    for ok, done in pending:
        when(ok, done)
    mixed = ALPHA * out_ref[...].astype(F32) + 0.5 * scatter_wait(2)
    current[...] = mixed
    stats_start(3, mixed)
    center, scale = stats_wait(3, features)
    out_ref[...] = ((current[...] - center) * scale * third_gain[...].astype(F32)).astype(BF16)


def solution(mesh):
    n_fs, n_tp = mesh.shape["fs"], mesh.shape["tp"]
    n_y = 1 << ((n_fs.bit_length() - 1) // 2)
    if n_fs % n_y:
        n_y = 1

    def body(
        tokens, first_gate, first_up, first_down, first_gain, glu_value, glu_gate, conv_taps, conv_gain,
        conv_proj, second_gain, last_gate, last_up, last_down, third_gain,
    ):
        current = tokens[0]
        length, width = current.shape
        weights = (first_gate, first_up, first_down, glu_value, glu_gate, conv_proj, last_gate, last_up, last_down)
        down = (2, 5, 8)
        cuts = (halves, halves, halves, whole, whole, whole, half_swapped, halves, halves)
        pieces = plan_pieces([(w.shape[0], cut) for w, cut in zip(weights, cuts)])
        n_z = n_fs // n_y
        first_slots = 2 * (max(n_z, n_y) - 1)
        second_slots = 2 * max(
            (1 + 2 * (n_z - 1)) * (n_y - 1),
            (1 + 2 * (n_y - 1)) * (n_z - 1),
        )
        channels = glu_value.shape[1]
        reach = (conv_taps.shape[0] - 1) // 2
        margin = -(-reach // 8) * 8
        bufs = [
            pltpu.VMEM((n_fs,) + w.shape if i in down else (n_fs * w.shape[0], w.shape[1]), BF16)
            for i, w in enumerate(weights)
        ]
        dma = pltpu.SemaphoreType.DMA
        vmem = pl.BlockSpec(memory_space=pltpu.VMEM)
        result = pl.pallas_call(
            functools.partial(layer_kernel, n_fs, n_tp, n_y, pieces),
            out_shape=jax.ShapeDtypeStruct((length, width), BF16),
            in_specs=[vmem] + [pl.BlockSpec(memory_space=pl.ANY)] * 9 + [vmem] * 5,
            out_specs=vmem,
            scratch_shapes=bufs
            + [
                pltpu.VMEM((3, length, width * n_tp), BF16),
                pltpu.VMEM((3, n_tp - 1, length, width), BF16),
                pltpu.VMEM((n_tp, length, width), BF16),
                pltpu.VMEM((length, first_gate.shape[1]), BF16),
                pltpu.VMEM((length, width), F32),
                pltpu.VMEM((length + 2 * margin, channels), F32),
                pltpu.VMEM((length, channels), BF16),
                pltpu.VMEM((4, n_tp, 8, length), F32),
                dma((len(pieces), first_slots)),
                dma((len(pieces), first_slots)),
                dma((len(pieces), second_slots)),
                dma((len(pieces), second_slots)),
                dma((len(pieces),)),
                dma((3, n_tp - 1)),
                dma((3, n_tp - 1)),
                dma((3, n_tp - 1)),
                dma((3, n_tp - 1)),
                dma((4, n_tp - 1)),
                dma((4, n_tp - 1)),
            ],
            compiler_params=pltpu.CompilerParams(
                collective_id=0, has_side_effects=True, vmem_limit_bytes=67000000
            ),
        )(
            current, *weights, first_gain[None], conv_taps, conv_gain[None], second_gain[None], third_gain[None]
        )
        return result[None]

    weight = P("fs", "tp")
    return jax.shard_map(
        body,
        mesh=mesh,
        in_specs=(
            P("fs", None, "tp"), weight, weight, P("tp", "fs"), P("tp"), weight, weight, P(None, "tp"), P("tp"),
            P("tp", "fs"), P("tp"), weight, weight, P("tp", "fs"), P("tp"),
        ),
        out_specs=P("fs", None, "tp"),
        check_vma=False,
    )
```

```python
import functools

import jax
import jax.numpy as jnp
from jax import lax
from jax.experimental import pallas as pl
from jax.experimental.pallas import tpu as pltpu
from jax.sharding import PartitionSpec as P

ALPHA = 2.0**0.25
EPSILON = 1e-05
MESH = pl.DeviceIdType.MESH
F32 = jnp.float32
BF16 = jnp.bfloat16


AHEAD_FIRST = 2
AHEAD_OWN = 1


def split_rows(rows, parts, step=16):
    swapped = max(step, (rows // 6 + step // 2) // step * step)
    units = (rows - swapped) // step
    sizes = [(units * (i + 1) // parts - units * i // parts) * step for i in range(parts)]
    return sizes, swapped


def plan_pieces(shapes, down, small, last):
    pieces = []
    for matrix, (rows, columns) in enumerate(shapes):
        if matrix in small:
            flip = matrix in down
            half = rows // 2
            pieces.append((matrix, 0, half, 0, columns, flip))
            pieces.append((matrix, half, half, 0, columns, False))
            continue
        wide = min(columns, 128) if matrix == last else columns
        for left in range(0, columns, wide):
            sizes, swapped = split_rows(rows, 2)
            order = [(sizes[0], False), (swapped, True)] + [(size, False) for size in sizes[1:]]
            start = 0
            for size, flip in order:
                pieces.append((matrix, start, size, left, wide, flip))
                start += size
    return pieces


def layer_kernel(
    n_fs,
    n_tp,
    n_y,
    pieces,
    tokens_ref,
    *refs,
):
    weights = refs[:9]
    first_gain, conv_taps, conv_gain, second_gain, third_gain = refs[9:14]
    out_ref = refs[14]
    bufs = refs[15:24]
    (xg, rs, send_buf, hidden, current, conv_in, acted, stat, z_s, z_r, y_s, y_r, loc_s, ag_s, ag_r, rs_s, rs_r, st_s, st_r, last_s, last_r) = refs[24:]

    n_z = n_fs // n_y
    fs = lax.axis_index("fs")
    tp = lax.axis_index("tp")
    z, y = fs // n_y, fs % n_y
    length, width = tokens_ref.shape
    features = width * n_tp

    barrier = pltpu.get_barrier_semaphore()
    for other in range(n_fs):
        @pl.when(other != fs)
        def _():
            pl.semaphore_signal(barrier, inc=1, device_id=(other, tp), device_id_type=MESH)
    for step in range(1, n_tp):
        pl.semaphore_signal(barrier, inc=1, device_id=(fs, (tp + step) % n_tp), device_id_type=MESH)
    pl.semaphore_wait(barrier, n_fs - 1 + n_tp - 1)

    pending = []

    def slot(c, block):
        matrix, start, size, left, wide, _ = pieces[c]
        buf = bufs[matrix]
        if len(buf.shape) == 2:
            rows = weights[matrix].shape[0]
            return buf.at[pl.ds(pl.multiple_of(block * rows + start, 16), size)]
        return buf.at[block, pl.ds(start, size), pl.ds(left, wide)]

    def own_rows(c):
        matrix, start, size, left, wide, _ = pieces[c]
        return weights[matrix].at[pl.ds(start, size), pl.ds(left, wide)]

    def remote(src, dst, s, r, dest):
        return pltpu.make_async_remote_copy(
            src_ref=src, dst_ref=dst, send_sem=s, recv_sem=r, device_id=dest, device_id_type=MESH
        )

    def axes(swapped):
        major, minor = (z, n_z, n_y), (y, n_y, 1)
        return (minor, major) if swapped else (major, minor)

    def when(cond, fn):
        pl.when(cond)(fn)

    def place(c, k, d, side):
        _, (_, extent, _) = axes(pieces[c][5])
        return (k * (extent - 1) + d - 1) * 2 + side

    def second_send(c, k, block, src):
        swapped = pieces[c][5]
        _, (pos, extent, stride) = axes(swapped)
        for side, sign in ((0, 1), (1, -1)):
            ok = pos < extent - 1 if side == 0 else pos > 0

            def go(side=side, sign=sign):
                i = place(c, k, 1, side)
                remote(src, slot(c, block), y_s.at[c, i], y_r.at[c, i], (fs + sign * stride, tp)).start()

            def done(side=side, sign=sign):
                i = place(c, k, 1, side)
                remote(src, slot(c, block), y_s.at[c, i], y_r.at[c, i], (fs + sign * stride, tp)).wait_send()

            when(ok, go)
            pending.append((ok, done))

    def own(c):
        swapped = pieces[c][5]
        src = own_rows(c)
        (pos, extent, stride), _ = axes(swapped)
        for side, sign in ((0, 1), (1, -1)):
            ok = pos < extent - 1 if side == 0 else pos > 0

            def copy(side=side, sign=sign):
                return remote(src, slot(c, fs), z_s.at[c, side], z_r.at[c, side], (fs + sign * stride, tp))

            when(ok, lambda copy=copy: copy().start())
            pending.append((ok, lambda copy=copy: copy().wait_send()))
        second_send(c, 0, fs, src)
        pltpu.make_async_copy(src, slot(c, fs), loc_s.at[c]).start()

    def first_axis(c):
        swapped = pieces[c][5]
        (pos, extent, stride), _ = axes(swapped)
        for d in range(1, extent):
            for side, sign in ((0, 1), (1, -1)):
                here = pos - sign * d >= 0 if side == 0 else pos + d < extent
                onward = here & (pos < extent - 1 if side == 0 else pos > 0)
                block = fs - sign * d * stride
                i = (d - 1) * 2 + side

                def arrive(block=block, i=i):
                    dst = slot(c, block)
                    remote(dst, dst, z_s.at[c, i], z_r.at[c, i], (fs, tp)).wait_recv()

                when(here, arrive)
                if d < extent - 1:
                    def copy(block=block, i=i, sign=sign):
                        dst = slot(c, block)
                        return remote(dst, dst, z_s.at[c, i + 2], z_r.at[c, i + 2], (fs + sign * stride, tp))

                    when(onward, lambda copy=copy: copy().start())
                    pending.append((onward, lambda copy=copy: copy().wait_send()))
                k = 1 + i
                _, (pos2, extent2, stride2) = axes(swapped)
                for side2, sign2 in ((0, 1), (1, -1)):
                    ok = here & (pos2 < extent2 - 1 if side2 == 0 else pos2 > 0)

                    def copy2(block=block, k=k, side2=side2, sign2=sign2, stride2=stride2):
                        j = place(c, k, 1, side2)
                        dst = slot(c, block)
                        return remote(dst, dst, y_s.at[c, j], y_r.at[c, j], (fs + sign2 * stride2, tp))

                    when(ok, lambda copy2=copy2: copy2().start())
                    pending.append((ok, lambda copy2=copy2: copy2().wait_send()))
                yield

    def second_axis(c):
        swapped = pieces[c][5]
        (pos, extent, stride), (pos2, extent2, stride2) = axes(swapped)
        origins = [(0, None, 0)] + [
            (1 + (d - 1) * 2 + side, side, d) for d in range(1, extent) for side in (0, 1)
        ]
        for d2 in range(1, extent2):
            for k, side, d in origins:
                if side is None:
                    here, first = True, fs
                else:
                    sign = 1 if side == 0 else -1
                    here = pos - d >= 0 if side == 0 else pos + d < extent
                    first = fs - sign * d * stride
                for side2, sign2 in ((0, 1), (1, -1)):
                    got = here & (pos2 - d2 >= 0 if side2 == 0 else pos2 + d2 < extent2)
                    block = first - sign2 * d2 * stride2
                    i = place(c, k, d2, side2)

                    def arrive(block=block, i=i):
                        dst = slot(c, block)
                        remote(dst, dst, y_s.at[c, i], y_r.at[c, i], (fs, tp)).wait_recv()

                    when(got, arrive)
                    if d2 < extent2 - 1:
                        ok = got & (pos2 < extent2 - 1 if side2 == 0 else pos2 > 0)

                        def copy(block=block, i=i, sign2=sign2):
                            dst = slot(c, block)
                            return remote(dst, dst, y_s.at[c, i + 2], y_r.at[c, i + 2], (fs + sign2 * stride2, tp))

                        when(ok, lambda copy=copy: copy().start())
                        pending.append((ok, lambda copy=copy: copy().wait_send()))
            yield
        pltpu.make_async_copy(own_rows(c), slot(c, fs), loc_s.at[c]).wait()

    landed = [0]

    def stream():
        count = len(pieces)
        lead = AHEAD_FIRST + AHEAD_OWN
        for c in range(min(lead, count)):
            own(c)
        yield
        for c in range(min(AHEAD_FIRST, count)):
            yield from first_axis(c)
        for c in range(count):
            if c + lead < count:
                own(c + lead)
            if c + AHEAD_FIRST < count:
                yield from first_axis(c + AHEAD_FIRST)
            yield from second_axis(c)
            landed[0] = c + 1
            yield

    pump_state = stream()

    def pump(steps):
        for _ in range(steps):
            next(pump_state, None)

    def until(matrix, right=None):
        need = 1 + max(
            i for i, piece in enumerate(pieces)
            if piece[0] == matrix and (right is None or piece[3] + piece[4] <= right)
        )
        while landed[0] < need:
            next(pump_state)

    def my_columns():
        return pl.ds(pl.multiple_of(tp * width, 128), width)

    def gather_start(phase, src):
        dst = xg.at[phase, :, my_columns()]
        for step in range(1, n_tp):
            i = step - 1
            remote(src, dst, ag_s.at[phase, i], ag_r.at[phase, i], (fs, (tp + step) % n_tp)).start()

    def gather_wait(phase, src):
        for step in range(1, n_tp):
            i = step - 1
            remote(src, src, ag_s.at[phase, i], ag_r.at[phase, i], (fs, tp)).wait()

    def scatter_start(phase):
        for step in range(1, n_tp):
            i = step - 1
            to = (tp + step) % n_tp
            remote(send_buf.at[to], rs.at[phase, i], rs_s.at[phase, i], rs_r.at[phase, i], (fs, to)).start()

    def scatter_columns(left, wide, part):
        copies = []
        n = left // wide
        for step in range(1, n_tp):
            i = step - 1
            to = (tp + step) % n_tp
            for q in range(width // part):
                cols = pl.ds(q * part + left, wide)
                j = (i * (part // wide) + n) * (width // part) + q
                copy = remote(
                    send_buf.at[to, :, cols], rs.at[2, i, :, cols], last_s.at[j], last_r.at[j], (fs, to)
                )
                copy.start()
                copies.append(copy)
        return copies

    def scatter_total(phase):
        total = send_buf[pl.ds(tp, 1)][0].astype(F32)
        for i in range(n_tp - 1):
            total = total + rs[phase, i].astype(F32)
        return total

    def scatter_wait(phase):
        for step in range(1, n_tp):
            i = step - 1
            remote(send_buf.at[0], rs.at[phase, i], rs_s.at[phase, i], rs_r.at[phase, i], (fs, tp)).wait()
        return scatter_total(phase)

    def stats_start(phase, values):
        sums = jnp.sum(values, axis=-1, keepdims=True)
        squares = jnp.sum(values * values, axis=-1, keepdims=True)
        lane = lax.broadcasted_iota(jnp.int32, (values.shape[0], 128), 1)
        both = jnp.where(lane == 0, sums, jnp.where(lane == 1, squares, 0.0))
        stat[phase, n_tp - 1] = both.T[:8]
        for step in range(1, n_tp):
            i = step - 1
            remote(
                stat.at[phase, n_tp - 1], stat.at[phase, i], st_s.at[phase, i], st_r.at[phase, i],
                (fs, (tp + step) % n_tp),
            ).start()

    def stats_wait(phase, all_width):
        for step in range(1, n_tp):
            i = step - 1
            remote(
                stat.at[phase, n_tp - 1], stat.at[phase, i], st_s.at[phase, i], st_r.at[phase, i], (fs, tp)
            ).wait()
        total = stat[phase, 0]
        for i in range(1, n_tp):
            total = total + stat[phase, i]
        both = jnp.concatenate([total] * 16, axis=0).T
        center = both[:, 0:1] / all_width
        spread = both[:, 1:2] / all_width - center * center
        return center, lax.rsqrt(spread + EPSILON)

    def ffn_hidden(phase, gate, up):
        tile = min(256, gate.shape[1])

        def step(j, carry):
            cols = pl.ds(pl.multiple_of(j * tile, 128), tile)
            held = xg[phase]
            g = jnp.dot(held, gate[:, cols], preferred_element_type=F32)
            u = jnp.dot(held, up[:, cols], preferred_element_type=F32)
            hidden[:, cols] = (g * jax.nn.sigmoid(g) * u).astype(BF16)
            return carry

        lax.fori_loop(0, gate.shape[1] // tile, step, 0)

    def project(source, buf, left=0, wide=None):
        part = buf.shape[2]
        per = width // part
        wide = wide or part

        def step(t, carry):
            held = source[...]
            for q in range(per):
                send_buf[t, :, q * part + left : q * part + left + wide] = jnp.dot(
                    held, buf[t * per + q, :, left : left + wide], preferred_element_type=F32
                ).astype(BF16)
            return carry

        lax.fori_loop(0, n_tp, step, 0)

    pump(1)
    xg[0, :, my_columns()] = tokens_ref[...]
    gather_start(0, tokens_ref)
    until(0)
    gather_wait(0, tokens_ref)
    until(1)
    ffn_hidden(0, bufs[0], bufs[1])
    until(2)
    project(hidden, bufs[2])
    scatter_start(0)
    pump(6)
    mixed = ALPHA * tokens_ref[...].astype(F32) + 0.5 * scatter_wait(0)
    current[...] = mixed
    stats_start(0, mixed)
    pump(4)
    center, scale = stats_wait(0, features)
    first = ((current[...] - center) * scale * first_gain[...].astype(F32)).astype(BF16)
    out_ref[...] = first
    xg[1, :, my_columns()] = first
    gather_start(1, out_ref)
    until(4)
    gather_wait(1, out_ref)

    channels = acted.shape[1]
    taps = conv_taps.shape[0]
    reach = (taps - 1) // 2
    margin = (conv_in.shape[0] - length) // 2
    held = xg[1]
    value = jnp.dot(held, bufs[3][...], preferred_element_type=F32)
    gate = jnp.dot(held, bufs[4][...], preferred_element_type=F32)
    conv_in[0:margin] = jnp.zeros((margin, channels), F32)
    conv_in[margin + length :] = jnp.zeros((margin, channels), F32)
    conv_in[margin : margin + length] = value * jax.nn.sigmoid(gate)
    pump(2)
    rows_each = length // 4
    for low in range(0, length, rows_each):
        for left in range(0, channels, 128):
            cols = slice(left, left + 128)
            total = jnp.zeros((rows_each, 128), F32)
            for tap in range(taps):
                start = margin - reach + low + tap
                total = total + conv_taps[tap : tap + 1, cols].astype(F32) * conv_in[start : start + rows_each, cols]
            current[low : low + rows_each, cols] = total
    stats_start(1, current[:, 0:channels])
    pump(4)
    center, scale = stats_wait(1, channels * n_tp)
    normed = (current[:, 0:channels] - center) * scale * conv_gain[...].astype(F32)
    acted[...] = (normed * jax.nn.sigmoid(normed)).astype(BF16)
    until(5)
    project(acted, bufs[5])
    scatter_start(1)
    pump(4)
    mixed = ALPHA * out_ref[...].astype(F32) + scatter_wait(1)
    current[...] = mixed
    stats_start(2, mixed)
    pump(4)
    center, scale = stats_wait(2, features)
    second = ((current[...] - center) * scale * second_gain[...].astype(F32)).astype(BF16)
    out_ref[...] = second
    xg[2, :, my_columns()] = second
    gather_start(2, out_ref)
    pump(4)
    gather_wait(2, out_ref)

    until(7)
    ffn_hidden(2, bufs[6], bufs[7])
    part = bufs[8].shape[2]
    wide = min(part, 128)
    copies = []
    for left in range(0, part, wide):
        until(8, left + wide)
        project(hidden, bufs[8], left, wide)
        copies += scatter_columns(left, wide, part)
    for _ in pump_state:
        pass
    for ok, done in pending:
        when(ok, done)
    for copy in copies:
        copy.wait()
    mixed = ALPHA * out_ref[...].astype(F32) + 0.5 * scatter_total(2)
    current[...] = mixed
    stats_start(3, mixed)
    center, scale = stats_wait(3, features)
    out_ref[...] = ((current[...] - center) * scale * third_gain[...].astype(F32)).astype(BF16)


def solution(mesh):
    n_fs, n_tp = mesh.shape["fs"], mesh.shape["tp"]
    n_y = 1 << ((n_fs.bit_length() - 1) // 2)
    if n_fs % n_y:
        n_y = 1

    def body(
        tokens, first_gate, first_up, first_down, first_gain, glu_value, glu_gate, conv_taps, conv_gain,
        conv_proj, second_gain, last_gate, last_up, last_down, third_gain,
    ):
        current = tokens[0]
        length, width = current.shape
        weights = (first_gate, first_up, first_down, glu_value, glu_gate, conv_proj, last_gate, last_up, last_down)
        down = (2, 5, 8)
        pieces = plan_pieces([w.shape for w in weights], down, (3, 4, 5), 8)
        n_z = n_fs // n_y
        first_slots = 2 * (max(n_z, n_y) - 1)
        second_slots = 2 * max(
            (1 + 2 * (n_z - 1)) * (n_y - 1),
            (1 + 2 * (n_y - 1)) * (n_z - 1),
        )
        channels = glu_value.shape[1]
        reach = (conv_taps.shape[0] - 1) // 2
        margin = -(-reach // 8) * 8
        n_last = (n_tp - 1) * (width // min(last_down.shape[1], 128))
        bufs = [
            pltpu.VMEM((n_fs,) + w.shape if i in down else (n_fs * w.shape[0], w.shape[1]), BF16)
            for i, w in enumerate(weights)
        ]
        dma = pltpu.SemaphoreType.DMA
        vmem = pl.BlockSpec(memory_space=pltpu.VMEM)
        result = pl.pallas_call(
            functools.partial(layer_kernel, n_fs, n_tp, n_y, pieces),
            out_shape=jax.ShapeDtypeStruct((length, width), BF16),
            in_specs=[vmem] + [pl.BlockSpec(memory_space=pl.ANY)] * 9 + [vmem] * 5,
            out_specs=vmem,
            scratch_shapes=bufs
            + [
                pltpu.VMEM((3, length, width * n_tp), BF16),
                pltpu.VMEM((3, n_tp - 1, length, width), BF16),
                pltpu.VMEM((n_tp, length, width), BF16),
                pltpu.VMEM((length, first_gate.shape[1]), BF16),
                pltpu.VMEM((length, width), F32),
                pltpu.VMEM((length + 2 * margin, channels), F32),
                pltpu.VMEM((length, channels), BF16),
                pltpu.VMEM((4, n_tp, 8, length), F32),
                dma((len(pieces), first_slots)),
                dma((len(pieces), first_slots)),
                dma((len(pieces), second_slots)),
                dma((len(pieces), second_slots)),
                dma((len(pieces),)),
                dma((3, n_tp - 1)),
                dma((3, n_tp - 1)),
                dma((3, n_tp - 1)),
                dma((3, n_tp - 1)),
                dma((4, n_tp - 1)),
                dma((4, n_tp - 1)),
                dma((n_last,)),
                dma((n_last,)),
            ],
            compiler_params=pltpu.CompilerParams(
                collective_id=0, has_side_effects=True, vmem_limit_bytes=67000000
            ),
        )(
            current, *weights, first_gain[None], conv_taps, conv_gain[None], second_gain[None], third_gain[None]
        )
        return result[None]

    weight = P("fs", "tp")
    return jax.shard_map(
        body,
        mesh=mesh,
        in_specs=(
            P("fs", None, "tp"), weight, weight, P("tp", "fs"), P("tp"), weight, weight, P(None, "tp"), P("tp"),
            P("tp", "fs"), P("tp"), weight, weight, P("tp", "fs"), P("tp"),
        ),
        out_specs=P("fs", None, "tp"),
        check_vma=False,
    )
```
